32 devices in a mesh: kv: 16 (over z, y, x), tp: 2 (over core).
Axes of the slice: x: 2, y: 2, z: 4, core: 2. Of those that a mesh axis runs over, the one named last changes fastest.
Arguments:
- hidden_in: bfloat16 [256, 2048], P('kv', 'tp'), may hold values from -6 to 6
- first_gain: bfloat16 [2048], P('tp'), may hold values from 0.099609375 to 1.8984375
- first_gate_proj: bfloat16 [2048, 5632], P('tp', 'kv'), may hold values from -0.125 to 0.125
- first_up_proj: bfloat16 [2048, 5632], P('tp', 'kv'), may hold values from -0.125 to 0.125
- first_down_proj: bfloat16 [5632, 2048], P('kv', 'tp'), may hold values from -0.078125 to 0.078125
- mix_gain: bfloat16 [2048], replicated, may hold values from 0.099609375 to 1.8984375
- query_weight: bfloat16 [2048, 1024], P(None, 'tp'), may hold values from -0.125 to 0.125
- forget_weight: bfloat16 [2048, 1024], P(None, 'tp'), may hold values from -0.125 to 0.125
- input_weight: bfloat16 [2048, 1024], P(None, 'tp'), may hold values from -0.125 to 0.125
- outgate_weight: bfloat16 [2048, 1024], P(None, 'tp'), may hold values from -0.125 to 0.125
- forget_floor: float32 [1024], P('tp'), may hold values from 0.05 to 0.95
- state_in: float32 [256, 8, 128, 128], P('kv', 'tp'), may hold values from -6 to 6
- out_gain: bfloat16 [1024], P('tp'), may hold values from 0.099609375 to 1.8984375
- mix_out_weight: bfloat16 [1024, 2048], P('tp'), may hold values from -0.1875 to 0.1875
- second_gain: bfloat16 [2048], P('tp'), may hold values from 0.099609375 to 1.8984375
- second_gate_proj: bfloat16 [2048, 5632], P('tp', 'kv'), may hold values from -0.125 to 0.125
- second_up_proj: bfloat16 [2048, 5632], P('tp', 'kv'), may hold values from -0.125 to 0.125
- second_down_proj: bfloat16 [5632, 2048], P('kv', 'tp'), may hold values from -0.078125 to 0.078125
Outputs:
- hidden_out: bfloat16 [256, 2048], P('kv', 'tp')
- state_out: float32 [256, 8, 128, 128], P('kv', 'tp')
The draws below stay inside these ranges and needn't reach their ends.
All inputs are finite; a program needn't handle non-finite values.
Results may differ from the reference program's by a relative error of at most 0.019.
Values may be sent and summed in bfloat16 or wider, within the bound.
A program may use at most 64 MiB of HBM per device.

```python
import jax
import jax.numpy as jnp
from jax import lax

D = 2048
FF = 5632
HEADS = 8
HEAD = 128
BATCH = 256
HK = 1024
N_TP = 2


def levels(stream_key, shape, pieces, low, high):
    def one(position, parts):
        draws = jax.random.uniform(jax.random.fold_in(jax.random.fold_in(stream_key, 6), position), (parts,), jnp.float32, low / len(pieces), high / len(pieces))
        return jnp.repeat(jnp.exp(draws), shape[position] // parts).reshape((-1,) + (1,) * (len(shape) - position - 1))

    loudness = one(*pieces[0])
    for cut in pieces[1:]:
        loudness = loudness * one(*cut)
    return loudness


def gaussian(key, shape, scale, most, pieces=(), dtype=jnp.bfloat16):
    level = levels(key, shape, pieces, -0.22, 0.18) if pieces else 1.0
    result = jax.random.normal(key, shape, jnp.float32) * scale * level
    return jnp.minimum(jnp.maximum(result, -most), most).astype(dtype)


def setup_inputs(seed: int = 0) -> dict:
    arg_keys = jax.random.split(jax.random.key(seed), 19)
    return {
        "hidden_in": gaussian(arg_keys[0], (BATCH, D), 1.0, 6.0, ((0, 16), (1, 2))),
        "first_gain": jnp.clip(1.0 + 0.18 * jax.random.normal(arg_keys[1], (D,), jnp.float32), 0.099609375, 1.8984375).astype(jnp.bfloat16),
        "first_gate_proj": gaussian(arg_keys[2], (D, FF), D ** -0.5, 0.125, ((0, 2), (1, 16))),
        "first_up_proj": gaussian(arg_keys[3], (D, FF), D ** -0.5, 0.125, ((0, 2), (1, 16))),
        "first_down_proj": gaussian(arg_keys[4], (FF, D), FF ** -0.5, 0.078125, ((0, 16), (1, 2))),
        "mix_gain": jnp.clip(1.0 + 0.18 * jax.random.normal(arg_keys[5], (D,), jnp.float32), 0.099609375, 1.8984375).astype(jnp.bfloat16),
        "query_weight": gaussian(arg_keys[6], (D, HK), D ** -0.5, 0.125, ((1, 2),)),
        "forget_weight": gaussian(arg_keys[7], (D, HK), D ** -0.5, 0.125, ((1, 2),)),
        "input_weight": gaussian(arg_keys[8], (D, HK), D ** -0.5, 0.125, ((1, 2),)),
        "outgate_weight": gaussian(arg_keys[9], (D, HK), D ** -0.5, 0.125, ((1, 2),)),
        "forget_floor": jnp.clip(0.05 + 0.9 * jax.random.uniform(arg_keys[10], (HK,), jnp.float32) ** levels(arg_keys[10], (HK,), ((0, 2),), -0.2, 0.2), 0.05, 0.95),
        "state_in": gaussian(arg_keys[11], (BATCH, HEADS, HEAD, HEAD), 1.0, 6.0, ((0, 16), (1, 2)), jnp.float32),
        "out_gain": jnp.clip(1.0 + 0.18 * jax.random.normal(arg_keys[12], (HK,), jnp.float32), 0.099609375, 1.8984375).astype(jnp.bfloat16),
        "mix_out_weight": gaussian(arg_keys[13], (HK, D), HK ** -0.5, 0.1875, ((0, 2),)),
        "second_gain": jnp.clip(1.0 + 0.18 * jax.random.normal(arg_keys[14], (D,), jnp.float32), 0.099609375, 1.8984375).astype(jnp.bfloat16),
        "second_gate_proj": gaussian(arg_keys[15], (D, FF), D ** -0.5, 0.125, ((0, 2), (1, 16))),
        "second_up_proj": gaussian(arg_keys[16], (D, FF), D ** -0.5, 0.125, ((0, 2), (1, 16))),
        "second_down_proj": gaussian(arg_keys[17], (FF, D), FF ** -0.5, 0.078125, ((0, 16), (1, 2))),
    }


def feed_forward(hidden, norm_gain, gate_proj, up_proj, down_proj):
    values = hidden.astype(jnp.float32)
    inverse = lax.rsqrt(lax.optimization_barrier(jnp.mean(values * values, axis=1, keepdims=True)) + 1e-06)
    scaled = (values * norm_gain.astype(jnp.float32)).astype(jnp.bfloat16)
    gate_sum = jnp.dot(scaled, gate_proj, preferred_element_type=jnp.float32) * inverse
    up_sum = jnp.dot(scaled, up_proj, preferred_element_type=jnp.float32) * inverse
    inner_units = (jax.nn.silu(gate_sum) * up_sum).astype(jnp.bfloat16)
    down_sum = jnp.dot(inner_units, down_proj, preferred_element_type=jnp.float32)
    return (values + 0.5 * down_sum).astype(jnp.bfloat16)

def reference(hidden_in, first_gain, first_gate_proj, first_up_proj, first_down_proj, mix_gain, query_weight, forget_weight, input_weight, outgate_weight, forget_floor, state_in, out_gain, mix_out_weight, second_gain, second_gate_proj, second_up_proj, second_down_proj):
    first_out = feed_forward(hidden_in, first_gain, first_gate_proj, first_up_proj, first_down_proj)
    values = first_out.astype(jnp.float32)
    inverse = lax.rsqrt(lax.optimization_barrier(jnp.mean(values * values, axis=1, keepdims=True)) + 1e-06)
    normed = (values * inverse * mix_gain.astype(jnp.float32)).astype(jnp.bfloat16)
    batch_size = hidden_in.shape[0]

    def project(weight):
        return jnp.dot(normed, weight, preferred_element_type=jnp.float32).reshape(batch_size, HEADS, HEAD)
    query_vals = jax.nn.silu(project(query_weight))
    forget_pre = project(forget_weight)
    input_vals = project(input_weight)
    out_gate = project(outgate_weight)
    floor_vals = forget_floor.reshape(HEADS, HEAD)
    log_forget = jnp.logaddexp(jnp.log(floor_vals), jnp.log1p(-floor_vals) + jax.nn.log_sigmoid(forget_pre))
    key_vals = -jnp.expm1(log_forget)
    new_state = jnp.exp(log_forget)[..., None] * state_in + key_vals[..., None] * input_vals[:, :, None, :]
    readout = jnp.einsum('bhk,bhkv->bhv', query_vals, new_state, precision=lax.Precision.HIGHEST)
    normed_out = readout * lax.rsqrt(lax.optimization_barrier(jnp.mean(readout * readout, axis=-1, keepdims=True)) + 1e-05) * out_gain.astype(jnp.float32).reshape(HEADS, HEAD)
    gated_out = (normed_out * jax.nn.silu(out_gate)).reshape(batch_size, HK).astype(jnp.bfloat16)
    group_width = HK // N_TP
    gated_groups = gated_out.reshape(batch_size, N_TP, group_width).astype(jnp.float32)
    weight_groups = mix_out_weight.reshape(N_TP, group_width, D).astype(jnp.float32)
    partial_value = jnp.einsum('bgk,gkd->bgd', gated_groups, weight_groups).astype(jnp.bfloat16)
    mixed_sum = lax.optimization_barrier(jnp.sum(partial_value.astype(jnp.float32), axis=1))
    second_in = (values + mixed_sum).astype(jnp.bfloat16)
    hidden_out = feed_forward(second_in, second_gain, second_gate_proj, second_up_proj, second_down_proj)
    return (hidden_out, new_state)
```

```python
import functools

import jax
import jax.numpy as jnp
from jax import lax
from jax.experimental import pallas as pl
from jax.experimental.pallas import tpu as pltpu
from jax.sharding import PartitionSpec as P

MESH = pl.DeviceIdType.MESH
F32 = jnp.float32
BF16 = jnp.bfloat16


def split_lines(count):
    lines = 1
    for guess in range(1, count + 1):
        if guess * guess <= count and count % guess == 0:
            lines = guess
    return lines, count // lines


def step_kernel(
    n_kv, n_tp,
    hid_hbm, vec_ref, gate1_hbm, up1_hbm, down1_hbm, wq_hbm, wf_hbm, wi_hbm, wo_hbm,
    state_hbm, wmix_hbm, gate2_hbm, up2_hbm, down2_hbm,
    out_ref, state_out_hbm,
    gate1, up1, down1, gate2, up2, down2, wq, wf, wi, wo, wmix, state,
    ag1, ag2, part1, part2, partin1, partin2, own, sq1, sq2, sqin1, sqin2,
    rs1, rs2, rsin1, rsin2, ownsum, line1, line2, linein1, linein2,
    rows_all, mix_send, mix_in, fs, qs, vs, ros,
    load_sem, local_sem, state_sem,
    line_s, line_r, plane_s, plane_r, tp_s, tp_r, tq_s, tq_r,
    rp_s, rp_r, rl_s, rl_r, row_s, row_r, mix_s, mix_r,
):
    n_l, n_p = split_lines(n_kv)
    rows, width = hid_hbm.shape
    depth = width * n_tp
    heads, head = state.shape[1], state.shape[2]
    kv = lax.axis_index("kv")
    tp = lax.axis_index("tp")
    ln = kv // n_p
    pn = kv % n_p

    def line_peer(d):
        return ((ln + d) % n_l) * n_p + pn

    def plane_peer(e):
        return ln * n_p + (pn + e) % n_p

    peers = (
        [(line_peer(d), tp) for d in range(1, n_l)]
        + [(plane_peer(e), tp) for e in range(1, n_p)]
        + [(kv, (tp + k) % n_tp) for k in range(1, n_tp)]
    )
    my_slot = pn * n_l + ln
    hid_copy = pltpu.make_async_copy(hid_hbm, ag1.at[my_slot], local_sem)
    hid_copy.start()
    loads = []
    for i, (src, dst) in enumerate(
        [
            (gate1_hbm, gate1), (up1_hbm, up1), (down1_hbm, down1),
            (wq_hbm, wq), (wf_hbm, wf), (wi_hbm, wi), (wo_hbm, wo),
            (state_hbm, state), (wmix_hbm, wmix),
            (gate2_hbm, gate2), (up2_hbm, up2), (down2_hbm, down2),
        ]
    ):
        copy = pltpu.make_async_copy(src, dst, load_sem.at[i])
        copy.start()
        loads.append(copy)
    barrier = pltpu.get_barrier_semaphore()
    for peer in peers:
        pl.semaphore_signal(barrier, inc=1, device_id=peer, device_id_type=MESH)
    pl.semaphore_wait(barrier, len(peers))
    sends = []

    def remote(src, dst, s, r, peer):
        return pltpu.make_async_remote_copy(
            src_ref=src, dst_ref=dst, send_sem=s, recv_sem=r, device_id=peer, device_id_type=MESH
        )

    def send(src, dst, s, r, peer):
        copy = remote(src, dst, s, r, peer)
        copy.start()
        sends.append(copy)

    def feed_forward(n, ag, gain, gate, up, down, part, partin, sq, sqin, rs, rsin, line, linein, w):
        own_row = (kv, tp)
        for e in range(1, n_p):
            send(ag.at[my_slot], ag.at[my_slot], plane_s.at[n, 0, e], plane_r.at[n, 0, e],
                 (plane_peer(e), tp))
        for d in range(1, n_l):
            send(ag.at[my_slot], ag.at[my_slot], line_s.at[n, d], line_r.at[n, d],
                 (line_peer(d), tp))
        for d in range(1, n_l):
            slot = pn * n_l + (ln + n_l - d) % n_l
            remote(ag.at[slot], ag.at[slot], line_s.at[n, d], line_r.at[n, d], own_row).wait_recv()
            for e in range(1, n_p):
                send(ag.at[slot], ag.at[slot], plane_s.at[n, d, e], plane_r.at[n, d, e],
                     (plane_peer(e), tp))
        w[0].wait()
        w[1].wait()
        for e in range(n_p):
            group = (pn + n_p - e) % n_p
            if e:
                for d in range(n_l):
                    slot = group * n_l + (ln + n_l - d) % n_l
                    remote(ag.at[slot], ag.at[slot], plane_s.at[n, d, e], plane_r.at[n, d, e],
                           own_row).wait_recv()
            values = ag[pl.ds(group * n_l, n_l)].reshape(n_l * rows, width).astype(F32)
            square = jnp.sum(values * values, axis=1, keepdims=True)
            sq[group] = jnp.broadcast_to(square, (n_l * rows, 128))
            scaled = (values * gain).astype(BF16)
            g = jnp.dot(scaled, gate[...], preferred_element_type=F32)
            own[group, 0] = g
            part[group, 0] = g.astype(BF16)
            u = jnp.dot(scaled, up[...], preferred_element_type=F32)
            own[group, 1] = u
            part[group, 1] = u.astype(BF16)
            for k in range(1, n_tp):
                peer = (kv, (tp + k) % n_tp)
                send(part.at[group], partin.at[k - 1, group], tp_s.at[n, e, k], tp_r.at[n, e, k], peer)
                send(sq.at[group], sqin.at[k - 1, group], tq_s.at[n, e, k], tq_r.at[n, e, k], peer)
        w[2].wait()
        for e in list(range(1, n_p)) + [0]:
            group = (pn + n_p - e) % n_p
            g = own[group, 0]
            u = own[group, 1]
            square = sq[group]
            for k in range(1, n_tp):
                remote(part.at[group], partin.at[k - 1, group], tp_s.at[n, e, k], tp_r.at[n, e, k],
                       own_row).wait_recv()
                remote(sq.at[group], sqin.at[k - 1, group], tq_s.at[n, e, k], tq_r.at[n, e, k],
                       own_row).wait_recv()
                g = g + partin[k - 1, group, 0].astype(F32)
                u = u + partin[k - 1, group, 1].astype(F32)
                square = square + sqin[k - 1, group]
            inverse = lax.rsqrt(square / depth + 1e-06)[:, :1]
            g = g * inverse
            h = (g / (1.0 + jnp.exp(-g)) * (u * inverse)).astype(BF16)
            y = jnp.dot(h, down[...], preferred_element_type=F32).reshape(n_l, rows, width)
            if e:
                rs[e - 1] = y.astype(BF16)
                for d in list(range(1, n_l)) + [0]:
                    place = (ln + d) % n_l
                    send(rs.at[e - 1, place], rsin.at[e - 1, place], rp_s.at[n, d, e],
                         rp_r.at[n, d, e], (ln * n_p + group, tp))
            else:
                ownsum[...] = y
        total = None
        for d in list(range(1, n_l)) + [0]:
            place = (ln + d) % n_l
            total = ownsum[place]
            for e in range(1, n_p):
                remote(rs.at[e - 1, place], rsin.at[e - 1, place], rp_s.at[n, d, e],
                       rp_r.at[n, d, e], own_row).wait_recv()
                total = total + rsin[e - 1, place].astype(F32)
            if d:
                line[d - 1] = total.astype(BF16)
                send(line.at[d - 1], linein.at[d - 1], rl_s.at[n, d], rl_r.at[n, d],
                     (line_peer(d), tp))
        for d in range(1, n_l):
            remote(line.at[d - 1], linein.at[d - 1], rl_s.at[n, d], rl_r.at[n, d],
                   own_row).wait_recv()
            total = total + linein[d - 1].astype(F32)
        return (ag[my_slot].astype(F32) + 0.5 * total).astype(BF16)

    hid_copy.wait()
    hw = heads * head
    gain1 = vec_ref[:, 0:width]
    gain2 = vec_ref[:, width : 2 * width]
    first_out = feed_forward(
        0, ag1, gain1, gate1, up1, down1, part1, partin1, sq1, sqin1, rs1, rsin1, line1, linein1,
        loads[0:3],
    )
    rows_all[tp] = first_out
    for k in range(1, n_tp):
        send(rows_all.at[tp], rows_all.at[tp], row_s.at[k], row_r.at[k], (kv, (tp + k) % n_tp))
    for copy in loads[3:7]:
        copy.wait()
    square = None
    sums = None
    for k in range(n_tp):
        t = (tp + n_tp - k) % n_tp
        if k:
            remote(rows_all.at[t], rows_all.at[t], row_s.at[k], row_r.at[k], (kv, tp)).wait_recv()
        values = rows_all[t].astype(F32)
        at = pl.multiple_of(t * width, 128)
        piece = jnp.sum(values * values, axis=1, keepdims=True)
        mixed = (values * vec_ref[:, pl.ds(2 * width + at, width)]).astype(BF16)
        terms = [
            jnp.dot(mixed, weight[pl.ds(at, width), :], preferred_element_type=F32)
            for weight in (wq, wf, wi, wo)
        ]
        square = piece if square is None else square + piece
        sums = terms if sums is None else [a + b for a, b in zip(sums, terms)]
    inverse = lax.rsqrt(square / depth + 1e-06)
    query, fpre, ival, ogate = [s * inverse for s in sums]
    query = query / (1.0 + jnp.exp(-query))
    ogate = ogate / (1.0 + jnp.exp(-ogate))
    base = 2 * width + depth
    floor = vec_ref[:, base : base + hw]
    out_gain = vec_ref[:, base + hw : base + 2 * hw]
    forget = floor + (1.0 - floor) / (1.0 + jnp.exp(-fpre))
    for h in range(heads):
        cut = slice(h * head, (h + 1) * head)
        qs[h] = query[:, cut]
        fs[h] = forget[:, cut]
        vs[h] = ival[:, cut]
    loads[7].wait()

    def one_head(h, carry):
        f_cols = fs[h].T
        q_cols = qs[h].T
        for b in range(rows):
            value = vs[h, b : b + 1, :]
            new = value + f_cols[:, b : b + 1] * (state[b, h] - value)
            state[b, h] = new
            ros[h, b : b + 1, :] = jnp.sum(q_cols[:, b : b + 1] * new, axis=0, keepdims=True)
        return carry

    lax.fori_loop(0, heads, one_head, 0)
    state_copy = pltpu.make_async_copy(state, state_out_hbm, state_sem)
    state_copy.start()
    loads[8].wait()
    mixed = None
    for h in range(heads):
        cut = slice(h * head, (h + 1) * head)
        read = ros[h]
        scale = lax.rsqrt(jnp.mean(read * read, axis=1, keepdims=True) + 1e-05)
        gated = (read * scale * out_gain[:, cut] * ogate[:, cut]).astype(BF16)
        term = jnp.dot(gated, wmix[cut, :], preferred_element_type=F32)
        mixed = term if mixed is None else mixed + term
    for t in range(n_tp):
        mix_send[t] = mixed[:, t * width : (t + 1) * width].astype(BF16)
    for k in range(1, n_tp):
        t = (tp + k) % n_tp
        send(mix_send.at[t], mix_in.at[k - 1], mix_s.at[k], mix_r.at[k], (kv, t))
    y2 = mix_send[tp].astype(F32)
    for k in range(1, n_tp):
        remote(mix_send.at[0], mix_in.at[k - 1], mix_s.at[k], mix_r.at[k], (kv, tp)).wait_recv()
        y2 = y2 + mix_in[k - 1].astype(F32)
    ag2[my_slot] = (rows_all[tp].astype(F32) + y2).astype(BF16)
    out_ref[...] = feed_forward(
        1, ag2, gain2, gate2, up2, down2, part2, partin2, sq2, sqin2, rs2, rsin2, line2, linein2,
        loads[9:12],
    )
    for copy in sends:
        copy.wait_send()
    state_copy.wait()


def shards(
    n_kv, n_tp,
    hidden_in, first_gain, first_gate_proj, first_up_proj, first_down_proj, mix_gain,
    query_weight, forget_weight, input_weight, outgate_weight, forget_floor, state_in,
    out_gain, mix_out_weight, second_gain, second_gate_proj, second_up_proj, second_down_proj,
):
    n_l, n_p = split_lines(n_kv)
    rows, width = hidden_in.shape
    units = first_gate_proj.shape[1]
    _, heads, head, _ = state_in.shape
    vec = jnp.concatenate(
        [v.astype(F32) for v in (first_gain, second_gain, mix_gain, forget_floor, out_gain)]
    )[None]
    v = pltpu.VMEM
    many = n_l * rows
    others = n_tp - 1

    def like(x):
        return v(x.shape, x.dtype)

    def two(shape, dtype):
        return [v(shape, dtype)] * 2

    dma = pltpu.SemaphoreType.DMA
    scratch = (
        [like(x) for x in (
            first_gate_proj, first_up_proj, first_down_proj,
            second_gate_proj, second_up_proj, second_down_proj,
            query_weight, forget_weight, input_weight, outgate_weight, mix_out_weight, state_in)]
        + two((n_kv, rows, width), BF16)
        + two((n_p, 2, many, units), BF16)
        + two((others, n_p, 2, many, units), BF16)
        + [v((n_p, 2, many, units), F32)]
        + two((n_p, many, 128), F32)
        + two((others, n_p, many, 128), F32)
        + two((n_p - 1, n_l, rows, width), BF16)
        + two((n_p - 1, n_l, rows, width), BF16)
        + [v((n_l, rows, width), F32)]
        + two((n_l - 1, rows, width), BF16)
        + two((n_l - 1, rows, width), BF16)
        + [v((n_tp, rows, width), BF16)] * 2
        + [v((others, rows, width), BF16)]
        + [v((heads, rows, head), F32)] * 4
        + [dma((12,)), dma, dma]
        + [dma((2, n_l))] * 2
        + [dma((2, n_l, n_p))] * 2
        + [dma((2, n_p, n_tp))] * 4
        + [dma((2, n_l, n_p))] * 2
        + [dma((2, n_l))] * 2
        + [dma((n_tp,))] * 4
    )
    hbm = pl.BlockSpec(memory_space=pl.ANY)
    vmem = pl.BlockSpec(memory_space=pltpu.VMEM)
    return pl.pallas_call(
        functools.partial(step_kernel, n_kv, n_tp),
        out_shape=(
            jax.ShapeDtypeStruct(hidden_in.shape, hidden_in.dtype),
            jax.ShapeDtypeStruct(state_in.shape, state_in.dtype),
        ),
        in_specs=[hbm, vmem] + [hbm] * 12,
        out_specs=(vmem, hbm),
        scratch_shapes=scratch,
        compiler_params=pltpu.CompilerParams(
            collective_id=0, has_side_effects=True, vmem_limit_bytes=60000 * 1024
        ),
    )(
        hidden_in, vec, first_gate_proj, first_up_proj, first_down_proj,
        query_weight, forget_weight, input_weight, outgate_weight,
        state_in, mix_out_weight, second_gate_proj, second_up_proj, second_down_proj,
    )


def solution(mesh):
    placed = (
        P("kv", "tp"), P("tp"), P("tp", "kv"), P("tp", "kv"), P("kv", "tp"), P(),
        P(None, "tp"), P(None, "tp"), P(None, "tp"), P(None, "tp"), P("tp"),
        P("kv", "tp", None, None), P("tp"), P("tp", None), P("tp"),
        P("tp", "kv"), P("tp", "kv"), P("kv", "tp"),
    )
    return jax.shard_map(
        functools.partial(shards, mesh.shape["kv"], mesh.shape["tp"]),
        mesh=mesh,
        in_specs=placed,
        out_specs=(P("kv", "tp"), P("kv", "tp", None, None)),
        check_vma=False,
    )
```

```python
import functools

import jax
import jax.numpy as jnp
from jax import lax
from jax.experimental import pallas as pl
from jax.experimental.pallas import tpu as pltpu
from jax.sharding import PartitionSpec as P

MESH = pl.DeviceIdType.MESH
F32 = jnp.float32
BF16 = jnp.bfloat16


def split_lines(count):
    lines = 1
    for guess in range(1, count + 1):
        if guess * guess <= count and count % guess == 0:
            lines = guess
    return lines, count // lines


def step_kernel(
    n_kv, n_tp,
    hid_hbm, gain1_ref, gain2_ref, gain_mix_ref, floor_ref, gain_out_ref, gate1_hbm, up1_hbm, down1_hbm, wq_hbm, wf_hbm, wi_hbm, wo_hbm,
    state_hbm, wmix_hbm, gate2_hbm, up2_hbm, down2_hbm,
    out_ref, state_out_hbm,
    gate1, up1, down1, gate2, up2, down2, wq, wf, wi, wo, wmix, state,
    ag1, ag2, part1, part2, partin1, partin2, own, sq1, sq2, sqin1, sqin2,
    rs1, rs2, rsin1, rsin2, ownsum, line1, line2, linein1, linein2,
    rows_all, mix_send, mix_in, fs, qs, vs, ros,
    load_sem, local_sem, state_sem,
    line_s, line_r, plane_s, plane_r, tp_s, tp_r, tq_s, tq_r,
    rp_s, rp_r, rl_s, rl_r, row_s, row_r, mix_s, mix_r,
):
    n_l, n_p = split_lines(n_kv)
    rows, width = hid_hbm.shape
    depth = width * n_tp
    heads, head = state.shape[1], state.shape[2]
    kv = lax.axis_index("kv")
    tp = lax.axis_index("tp")
    ln = kv // n_p
    pn = kv % n_p

    def line_peer(d):
        return ((ln + d) % n_l) * n_p + pn

    def plane_peer(e):
        return ln * n_p + (pn + e) % n_p

    peers = (
        [(line_peer(d), tp) for d in range(1, n_l)]
        + [(plane_peer(e), tp) for e in range(1, n_p)]
        + [(kv, (tp + k) % n_tp) for k in range(1, n_tp)]
    )
    my_slot = pn * n_l + ln
    hid_copy = pltpu.make_async_copy(hid_hbm, ag1.at[my_slot], local_sem)
    hid_copy.start()
    loads = []
    for i, (src, dst) in enumerate(
        [
            (gate1_hbm, gate1), (up1_hbm, up1), (down1_hbm, down1),
            (wq_hbm, wq), (wf_hbm, wf), (wi_hbm, wi), (wo_hbm, wo),
            (state_hbm, state), (wmix_hbm, wmix),
            (gate2_hbm, gate2), (up2_hbm, up2), (down2_hbm, down2),
        ]
    ):
        copy = pltpu.make_async_copy(src, dst, load_sem.at[i])
        copy.start()
        loads.append(copy)
    barrier = pltpu.get_barrier_semaphore()
    for peer in peers:
        pl.semaphore_signal(barrier, inc=1, device_id=peer, device_id_type=MESH)
    pl.semaphore_wait(barrier, len(peers))
    sends = []

    def remote(src, dst, s, r, peer):
        return pltpu.make_async_remote_copy(
            src_ref=src, dst_ref=dst, send_sem=s, recv_sem=r, device_id=peer, device_id_type=MESH
        )

    def send(src, dst, s, r, peer):
        copy = remote(src, dst, s, r, peer)
        copy.start()
        sends.append(copy)

    def wide_dot(a, b):
        return lax.dot_general(a, b, (((1,), (1,)), ((), ())), preferred_element_type=F32)

    def feed_forward(
        n, ag, gain, gate, up, down, part, partin, sq, sqin, rs, rsin, line, linein, w, fill
    ):
        own_row = (kv, tp)
        for e in range(1, n_p):
            send(ag.at[my_slot], ag.at[my_slot], plane_s.at[n, 0, e], plane_r.at[n, 0, e],
                 (plane_peer(e), tp))
        for d in range(1, n_l):
            send(ag.at[my_slot], ag.at[my_slot], line_s.at[n, d], line_r.at[n, d],
                 (line_peer(d), tp))
        if fill is not None:
            fill()
        for d in range(1, n_l):
            slot = pn * n_l + (ln + n_l - d) % n_l
            remote(ag.at[slot], ag.at[slot], line_s.at[n, d], line_r.at[n, d], own_row).wait_recv()
            for e in range(1, n_p):
                send(ag.at[slot], ag.at[slot], plane_s.at[n, d, e], plane_r.at[n, d, e],
                     (plane_peer(e), tp))
        w[0].wait()
        w[1].wait()
        w[2].wait()

        def stage_in(e):
            group = (pn + n_p - e) % n_p
            if e:
                for d in range(n_l):
                    slot = group * n_l + (ln + n_l - d) % n_l
                    remote(ag.at[slot], ag.at[slot], plane_s.at[n, d, e], plane_r.at[n, d, e],
                           own_row).wait_recv()
            values = ag[pl.ds(group * n_l, n_l)].reshape(n_l * rows, width).astype(F32)
            square = jnp.sum(values * values, axis=1, keepdims=True)
            sq[group] = jnp.broadcast_to(square, (n_l * rows, 128))
            scaled = (values * gain).astype(BF16)
            g = wide_dot(scaled, gate[...])
            own[group, 0] = g
            part[group, 0] = g.astype(BF16)
            u = wide_dot(scaled, up[...])
            own[group, 1] = u
            part[group, 1] = u.astype(BF16)
            for k in range(1, n_tp):
                peer = (kv, (tp + k) % n_tp)
                send(part.at[group], partin.at[k - 1, group], tp_s.at[n, e, k], tp_r.at[n, e, k], peer)
                send(sq.at[group], sqin.at[k - 1, group], tq_s.at[n, e, k], tq_r.at[n, e, k], peer)

        def stage_out(e):
            group = (pn + n_p - e) % n_p
            g = own[group, 0]
            u = own[group, 1]
            square = sq[group]
            for k in range(1, n_tp):
                remote(part.at[group], partin.at[k - 1, group], tp_s.at[n, e, k], tp_r.at[n, e, k],
                       own_row).wait_recv()
                remote(sq.at[group], sqin.at[k - 1, group], tq_s.at[n, e, k], tq_r.at[n, e, k],
                       own_row).wait_recv()
                g = g + partin[k - 1, group, 0].astype(F32)
                u = u + partin[k - 1, group, 1].astype(F32)
                square = square + sqin[k - 1, group]
            inverse = lax.rsqrt(square / depth + 1e-06)[:, :1]
            g = g * inverse
            h = (g / (1.0 + jnp.exp(-g)) * (u * inverse)).astype(BF16)
            y = jnp.dot(h, down[...], preferred_element_type=F32).reshape(n_l, rows, width)
            if e:
                rs[e - 1] = y.astype(BF16)
                for d in list(range(1, n_l)) + [0]:
                    place = (ln + d) % n_l
                    send(rs.at[e - 1, place], rsin.at[e - 1, place], rp_s.at[n, d, e],
                         rp_r.at[n, d, e], (ln * n_p + group, tp))
            else:
                ownsum[...] = y

        for e in range(n_p):
            stage_in(e)
            if e > 1:
                stage_out(e - 1)
        if n_p > 1:
            stage_out(n_p - 1)
        stage_out(0)
        total = None
        for d in list(range(1, n_l)) + [0]:
            place = (ln + d) % n_l
            total = ownsum[place]
            for e in range(1, n_p):
                remote(rs.at[e - 1, place], rsin.at[e - 1, place], rp_s.at[n, d, e],
                       rp_r.at[n, d, e], own_row).wait_recv()
                total = total + rsin[e - 1, place].astype(F32)
            if d:
                line[d - 1] = total.astype(BF16)
                send(line.at[d - 1], linein.at[d - 1], rl_s.at[n, d], rl_r.at[n, d],
                     (line_peer(d), tp))
        for d in range(1, n_l):
            remote(line.at[d - 1], linein.at[d - 1], rl_s.at[n, d], rl_r.at[n, d],
                   own_row).wait_recv()
            total = total + linein[d - 1].astype(F32)
        return (ag[my_slot].astype(F32) + 0.5 * total).astype(BF16)

    hid_copy.wait()
    hw = heads * head
    gain1 = gain1_ref[...].astype(F32).reshape(1, width)
    gain2 = gain2_ref[...].astype(F32).reshape(1, width)
    first_out = feed_forward(
        0, ag1, gain1, gate1, up1, down1, part1, partin1, sq1, sqin1, rs1, rsin1, line1, linein1,
        loads[0:3], None,
    )
    rows_all[tp] = first_out
    for k in range(1, n_tp):
        send(rows_all.at[tp], rows_all.at[tp], row_s.at[k], row_r.at[k], (kv, (tp + k) % n_tp))
    for copy in loads[3:7]:
        copy.wait()
    square = None
    sums = None
    for k in range(n_tp):
        t = (tp + n_tp - k) % n_tp
        if k:
            remote(rows_all.at[t], rows_all.at[t], row_s.at[k], row_r.at[k], (kv, tp)).wait_recv()
        values = rows_all[t].astype(F32)
        at = pl.multiple_of(t * width, 128)
        piece = jnp.sum(values * values, axis=1, keepdims=True)
        mixed = (values * gain_mix_ref[pl.ds(at, width)].astype(F32).reshape(1, width)).astype(BF16)
        terms = [
            jnp.dot(mixed, weight[pl.ds(at, width), :], preferred_element_type=F32)
            for weight in (wq, wf, wi, wo)
        ]
        square = piece if square is None else square + piece
        sums = terms if sums is None else [a + b for a, b in zip(sums, terms)]
    inverse = lax.rsqrt(square / depth + 1e-06)
    query, fpre, ival, ogate = [s * inverse for s in sums]
    query = query / (1.0 + jnp.exp(-query))
    ogate = ogate / (1.0 + jnp.exp(-ogate))
    floor = floor_ref[...].reshape(1, hw)
    out_gain = gain_out_ref[...].astype(F32).reshape(1, hw)
    forget = floor + (1.0 - floor) / (1.0 + jnp.exp(-fpre))
    for h in range(heads):
        cut = slice(h * head, (h + 1) * head)
        qs[h] = query[:, cut] * forget[:, cut]
        fs[h] = forget[:, cut]
        vs[h] = ival[:, cut]
    loads[7].wait()

    def read_head(h, carry):
        cols = qs[h].T
        for b in range(rows):
            ros[h, b : b + 1, :] = jnp.sum(
                cols[:, b : b + 1] * state[b, h], axis=0, keepdims=True
            )
        return carry

    lax.fori_loop(0, heads, read_head, 0)

    def update_state():
        def one_head(h, carry):
            cols = fs[h].T
            for b in range(rows):
                value = vs[h, b : b + 1, :]
                state[b, h] = value + cols[:, b : b + 1] * (state[b, h] - value)
            return carry

        lax.fori_loop(0, heads, one_head, 0)
        state_copy.start()

    state_copy = pltpu.make_async_copy(state, state_out_hbm, state_sem)
    loads[8].wait()
    mixed = None
    for h in range(heads):
        cut = slice(h * head, (h + 1) * head)
        inner = jnp.sum(query[:, cut] * (1.0 - forget[:, cut]), axis=1, keepdims=True)
        read = ros[h] + inner * ival[:, cut]
        scale = lax.rsqrt(jnp.mean(read * read, axis=1, keepdims=True) + 1e-05)
        gated = (read * scale * out_gain[:, cut] * ogate[:, cut]).astype(BF16)
        term = jnp.dot(gated, wmix[cut, :], preferred_element_type=F32)
        mixed = term if mixed is None else mixed + term
    for t in range(n_tp):
        mix_send[t] = mixed[:, t * width : (t + 1) * width].astype(BF16)
    for k in range(1, n_tp):
        t = (tp + k) % n_tp
        send(mix_send.at[t], mix_in.at[k - 1], mix_s.at[k], mix_r.at[k], (kv, t))
    y2 = mix_send[tp].astype(F32)
    for k in range(1, n_tp):
        remote(mix_send.at[0], mix_in.at[k - 1], mix_s.at[k], mix_r.at[k], (kv, tp)).wait_recv()
        y2 = y2 + mix_in[k - 1].astype(F32)
    ag2[my_slot] = (rows_all[tp].astype(F32) + y2).astype(BF16)
    out_ref[...] = feed_forward(
        1, ag2, gain2, gate2, up2, down2, part2, partin2, sq2, sqin2, rs2, rsin2, line2, linein2,
        loads[9:12], update_state,
    )
    for copy in sends:
        copy.wait_send()
    state_copy.wait()


def shards(
    n_kv, n_tp,
    hidden_in, first_gain, first_gate_proj, first_up_proj, first_down_proj, mix_gain,
    query_weight, forget_weight, input_weight, outgate_weight, forget_floor, state_in,
    out_gain, mix_out_weight, second_gain, second_gate_proj, second_up_proj, second_down_proj,
):
    n_l, n_p = split_lines(n_kv)
    rows, width = hidden_in.shape
    units = first_gate_proj.shape[1]
    _, heads, head, _ = state_in.shape
    first_gate_proj, first_up_proj, second_gate_proj, second_up_proj = [
        w.T for w in (first_gate_proj, first_up_proj, second_gate_proj, second_up_proj)
    ]
    v = pltpu.VMEM
    many = n_l * rows
    others = n_tp - 1

    def like(x):
        return v(x.shape, x.dtype)

    def two(shape, dtype):
        return [v(shape, dtype)] * 2

    dma = pltpu.SemaphoreType.DMA
    scratch = (
        [like(x) for x in (
            first_gate_proj, first_up_proj, first_down_proj,
            second_gate_proj, second_up_proj, second_down_proj,
            query_weight, forget_weight, input_weight, outgate_weight, mix_out_weight, state_in)]
        + two((n_kv, rows, width), BF16)
        + two((n_p, 2, many, units), BF16)
        + two((others, n_p, 2, many, units), BF16)
        + [v((n_p, 2, many, units), F32)]
        + two((n_p, many, 128), F32)
        + two((others, n_p, many, 128), F32)
        + two((n_p - 1, n_l, rows, width), BF16)
        + two((n_p - 1, n_l, rows, width), BF16)
        + [v((n_l, rows, width), F32)]
        + two((n_l - 1, rows, width), BF16)
        + two((n_l - 1, rows, width), BF16)
        + [v((n_tp, rows, width), BF16)] * 2
        + [v((others, rows, width), BF16)]
        + [v((heads, rows, head), F32)] * 4
        + [dma((12,)), dma, dma]
        + [dma((2, n_l))] * 2
        + [dma((2, n_l, n_p))] * 2
        + [dma((2, n_p, n_tp))] * 4
        + [dma((2, n_l, n_p))] * 2
        + [dma((2, n_l))] * 2
        + [dma((n_tp,))] * 4
    )
    hbm = pl.BlockSpec(memory_space=pl.ANY)
    vmem = pl.BlockSpec(memory_space=pltpu.VMEM)
    return pl.pallas_call(
        functools.partial(step_kernel, n_kv, n_tp),
        out_shape=(
            jax.ShapeDtypeStruct(hidden_in.shape, hidden_in.dtype),
            jax.ShapeDtypeStruct(state_in.shape, state_in.dtype),
        ),
        in_specs=[hbm] + [vmem] * 5 + [hbm] * 12,
        out_specs=(vmem, hbm),
        scratch_shapes=scratch,
        compiler_params=pltpu.CompilerParams(
            collective_id=0, has_side_effects=True, vmem_limit_bytes=60000 * 1024
        ),
    )(
        hidden_in, first_gain, second_gain, mix_gain, forget_floor, out_gain, first_gate_proj, first_up_proj, first_down_proj,
        query_weight, forget_weight, input_weight, outgate_weight,
        state_in, mix_out_weight, second_gate_proj, second_up_proj, second_down_proj,
    )


def solution(mesh):
    placed = (
        P("kv", "tp"), P("tp"), P("tp", "kv"), P("tp", "kv"), P("kv", "tp"), P(),
        P(None, "tp"), P(None, "tp"), P(None, "tp"), P(None, "tp"), P("tp"),
        P("kv", "tp", None, None), P("tp"), P("tp", None), P("tp"),
        P("tp", "kv"), P("tp", "kv"), P("kv", "tp"),
    )
    return jax.shard_map(
        functools.partial(shards, mesh.shape["kv"], mesh.shape["tp"]),
        mesh=mesh,
        in_specs=placed,
        out_specs=(P("kv", "tp"), P("kv", "tp", None, None)),
        check_vma=False,
    )
```

```python
import functools

import jax
import jax.numpy as jnp
from jax import lax
from jax.experimental import pallas as pl
from jax.experimental.pallas import tpu as pltpu
from jax.sharding import PartitionSpec as P

MESH = pl.DeviceIdType.MESH
F32 = jnp.float32
BF16 = jnp.bfloat16


def split_lines(count):
    lines = 1
    for guess in range(1, count + 1):
        if guess * guess <= count and count % guess == 0:
            lines = guess
    return lines, count // lines


def step_kernel(
    n_kv, n_tp,
    hid_hbm, gain1_ref, gain2_ref, gain_mix_ref, floor_ref, gain_out_ref, gate1_hbm, up1_hbm, down1_hbm, wq_hbm, wf_hbm, wi_hbm, wo_hbm,
    state_hbm, wmix_hbm, gate2_hbm, up2_hbm, down2_hbm,
    out_ref, fs, vs,
    gate1, up1, down1, gate2, up2, down2, wq, wf, wi, wo, wmix, state,
    ag1, ag2, part1, part2, partin1, partin2, own, sq1, sq2, sqin1, sqin2,
    rs1, rs2, rsin1, rsin2, ownsum, line1, line2, linein1, linein2,
    rows_all, mix_send, mix_in, qs, ros,
    load_sem, local_sem,
    line_s, line_r, plane_s, plane_r, tp_s, tp_r, tq_s, tq_r,
    rp_s, rp_r, rl_s, rl_r, row_s, row_r, mix_s, mix_r,
):
    n_l, n_p = split_lines(n_kv)
    rows, width = hid_hbm.shape
    depth = width * n_tp
    heads, head = state.shape[1], state.shape[2]
    kv = lax.axis_index("kv")
    tp = lax.axis_index("tp")
    ln = kv // n_p
    pn = kv % n_p

    def line_peer(place):
        return place * n_p + pn

    def plane_peer(e):
        return ln * n_p + (pn + e) % n_p

    low = 1 - (2 * ln) // n_l
    far_first = []
    for i in range(n_l - 1):
        down_from = n_l - 1 - i
        down_from = down_from - (ln - down_from + n_l) // n_l
        up_from = i + (i - ln + n_l) // n_l
        far_first.append(low * down_from + (1 - low) * up_from)
    near_first = far_first[::-1]

    peers = (
        [(line_peer(place), tp) for place in far_first]
        + [(plane_peer(e), tp) for e in range(1, n_p)]
        + [(kv, (tp + k) % n_tp) for k in range(1, n_tp)]
    )
    my_slot = pn * n_l + ln
    hid_copy = pltpu.make_async_copy(hid_hbm, ag1.at[my_slot], local_sem)
    hid_copy.start()
    loads = []
    for i, (src, dst) in enumerate(
        [
            (gate1_hbm, gate1), (up1_hbm, up1), (down1_hbm, down1),
            (wq_hbm, wq), (wf_hbm, wf), (wi_hbm, wi), (wo_hbm, wo),
            (state_hbm, state), (wmix_hbm, wmix),
            (gate2_hbm, gate2), (up2_hbm, up2), (down2_hbm, down2),
        ]
    ):
        loads.append(pltpu.make_async_copy(src, dst, load_sem.at[i]))
    barrier = pltpu.get_barrier_semaphore()
    for peer in peers:
        pl.semaphore_signal(barrier, inc=1, device_id=peer, device_id_type=MESH)
    pl.semaphore_wait(barrier, len(peers))
    sends = []

    def remote(src, dst, s, r, peer):
        return pltpu.make_async_remote_copy(
            src_ref=src, dst_ref=dst, send_sem=s, recv_sem=r, device_id=peer, device_id_type=MESH
        )

    def send(src, dst, s, r, peer):
        copy = remote(src, dst, s, r, peer)
        copy.start()
        sends.append(copy)

    def wide_dot(a, b):
        return lax.dot_general(a, b, (((1,), (1,)), ((), ())), preferred_element_type=F32)

    def feed_forward(
        n, ag, gain, gate, up, down, part, partin, sq, sqin, rs, rsin, line, linein, w, fill
    ):
        own_row = (kv, tp)
        for place in near_first:
            send(ag.at[my_slot], ag.at[my_slot], line_s.at[n, place], line_r.at[n, ln],
                 (line_peer(place), tp))
        for e in range(1, n_p):
            send(ag.at[my_slot], ag.at[my_slot], plane_s.at[n, ln, e], plane_r.at[n, ln, e],
                 (plane_peer(e), tp))
        if fill is not None:
            fill()
        for place in near_first:
            slot = pn * n_l + place
            remote(ag.at[slot], ag.at[slot], line_s.at[n, place], line_r.at[n, place],
                   own_row).wait_recv()
            for e in range(1, n_p):
                send(ag.at[slot], ag.at[slot], plane_s.at[n, place, e], plane_r.at[n, place, e],
                     (plane_peer(e), tp))
        w[0].wait()
        w[1].wait()
        w[2].wait()

        def stage_in(e):
            group = (pn + n_p - e) % n_p
            if e:
                for place in range(n_l):
                    slot = group * n_l + place
                    remote(ag.at[slot], ag.at[slot], plane_s.at[n, place, e], plane_r.at[n, place, e],
                           own_row).wait_recv()
            values = ag[pl.ds(group * n_l, n_l)].reshape(n_l * rows, width).astype(F32)
            square = jnp.sum(values * values, axis=1, keepdims=True)
            sq[group] = jnp.broadcast_to(square, (n_l * rows, 128))
            scaled = (values * gain).astype(BF16)
            g = wide_dot(scaled, gate[...])
            own[group, 0] = g
            part[group, 0] = g.astype(BF16)
            u = wide_dot(scaled, up[...])
            own[group, 1] = u
            part[group, 1] = u.astype(BF16)
            for k in range(1, n_tp):
                peer = (kv, (tp + k) % n_tp)
                send(part.at[group], partin.at[k - 1, group], tp_s.at[n, e, k], tp_r.at[n, e, k], peer)
                send(sq.at[group], sqin.at[k - 1, group], tq_s.at[n, e, k], tq_r.at[n, e, k], peer)

        def stage_out(e):
            group = (pn + n_p - e) % n_p
            g = own[group, 0]
            u = own[group, 1]
            square = sq[group]
            for k in range(1, n_tp):
                remote(part.at[group], partin.at[k - 1, group], tp_s.at[n, e, k], tp_r.at[n, e, k],
                       own_row).wait_recv()
                remote(sq.at[group], sqin.at[k - 1, group], tq_s.at[n, e, k], tq_r.at[n, e, k],
                       own_row).wait_recv()
                g = g + partin[k - 1, group, 0].astype(F32)
                u = u + partin[k - 1, group, 1].astype(F32)
                square = square + sqin[k - 1, group]
            inverse = lax.rsqrt(square / depth + 1e-06)[:, :1]
            g = g * inverse
            h = (g / (1.0 + jnp.exp(-g)) * (u * inverse)).astype(BF16)
            y = jnp.dot(h, down[...], preferred_element_type=F32).reshape(n_l, rows, width)
            if e:
                rs[e - 1] = y.astype(BF16)
                for place in far_first + [ln]:
                    send(rs.at[e - 1, place], rsin.at[e - 1, place], rp_s.at[n, place, e],
                         rp_r.at[n, place, e], (ln * n_p + group, tp))
            else:
                ownsum[...] = y

        for e in range(n_p):
            stage_in(e)
            if e > 1:
                stage_out(e - 1)
        if n_p > 1:
            stage_out(n_p - 1)
        stage_out(0)
        total = None
        for i, place in enumerate(far_first + [ln]):
            total = ownsum[place]
            for e in range(1, n_p):
                remote(rs.at[e - 1, place], rsin.at[e - 1, place], rp_s.at[n, place, e],
                       rp_r.at[n, place, e], own_row).wait_recv()
                total = total + rsin[e - 1, place].astype(F32)
            if i < n_l - 1:
                line[place] = total.astype(BF16)
                send(line.at[place], linein.at[ln], rl_s.at[n, place], rl_r.at[n, ln],
                     (line_peer(place), tp))
        for place in near_first:
            remote(line.at[place], linein.at[place], rl_s.at[n, place], rl_r.at[n, place],
                   own_row).wait_recv()
            total = total + linein[place].astype(F32)
        return (ag[my_slot].astype(F32) + 0.5 * total).astype(BF16)

    hid_copy.wait()

    def start_loads():
        for copy in loads:
            copy.start()

    hw = heads * head
    gain1 = gain1_ref[...].astype(F32).reshape(1, width)
    gain2 = gain2_ref[...].astype(F32).reshape(1, width)
    first_out = feed_forward(
        0, ag1, gain1, gate1, up1, down1, part1, partin1, sq1, sqin1, rs1, rsin1, line1, linein1,
        loads[0:3], start_loads,
    )
    rows_all[tp] = first_out
    for k in range(1, n_tp):
        send(rows_all.at[tp], rows_all.at[tp], row_s.at[k], row_r.at[k], (kv, (tp + k) % n_tp))
    for copy in loads[3:7]:
        copy.wait()
    square = None
    sums = None
    for k in range(n_tp):
        t = (tp + n_tp - k) % n_tp
        if k:
            remote(rows_all.at[t], rows_all.at[t], row_s.at[k], row_r.at[k], (kv, tp)).wait_recv()
        values = rows_all[t].astype(F32)
        at = pl.multiple_of(t * width, 128)
        piece = jnp.sum(values * values, axis=1, keepdims=True)
        mixed = (values * gain_mix_ref[pl.ds(at, width)].astype(F32).reshape(1, width)).astype(BF16)
        terms = [
            jnp.dot(mixed, weight[pl.ds(at, width), :], preferred_element_type=F32)
            for weight in (wq, wf, wi, wo)
        ]
        square = piece if square is None else square + piece
        sums = terms if sums is None else [a + b for a, b in zip(sums, terms)]
    inverse = lax.rsqrt(square / depth + 1e-06)
    query, fpre, ival, ogate = [s * inverse for s in sums]
    query = query / (1.0 + jnp.exp(-query))
    ogate = ogate / (1.0 + jnp.exp(-ogate))
    floor = floor_ref[...].reshape(1, hw)
    out_gain = gain_out_ref[...].astype(F32).reshape(1, hw)
    forget = floor + (1.0 - floor) / (1.0 + jnp.exp(-fpre))
    for h in range(heads):
        cut = slice(h * head, (h + 1) * head)
        qs[h] = query[:, cut] * forget[:, cut]
        fs[h] = forget[:, cut]
        vs[h] = ival[:, cut]
    loads[7].wait()

    def read_head(h, carry):
        cols = qs[h].T
        for b in range(rows):
            ros[h, b : b + 1, :] = jnp.sum(
                cols[:, b : b + 1] * state[b, h], axis=0, keepdims=True
            )
        return carry

    lax.fori_loop(0, heads, read_head, 0)
    loads[8].wait()
    mixed = None
    for h in range(heads):
        cut = slice(h * head, (h + 1) * head)
        inner = jnp.sum(query[:, cut] * (1.0 - forget[:, cut]), axis=1, keepdims=True)
        read = ros[h] + inner * ival[:, cut]
        scale = lax.rsqrt(jnp.mean(read * read, axis=1, keepdims=True) + 1e-05)
        gated = (read * scale * out_gain[:, cut] * ogate[:, cut]).astype(BF16)
        term = jnp.dot(gated, wmix[cut, :], preferred_element_type=F32)
        mixed = term if mixed is None else mixed + term
    for t in range(n_tp):
        mix_send[t] = mixed[:, t * width : (t + 1) * width].astype(BF16)
    for k in range(1, n_tp):
        t = (tp + k) % n_tp
        send(mix_send.at[t], mix_in.at[k - 1], mix_s.at[k], mix_r.at[k], (kv, t))
    y2 = mix_send[tp].astype(F32)
    for k in range(1, n_tp):
        remote(mix_send.at[0], mix_in.at[k - 1], mix_s.at[k], mix_r.at[k], (kv, tp)).wait_recv()
        y2 = y2 + mix_in[k - 1].astype(F32)
    ag2[my_slot] = (rows_all[tp].astype(F32) + y2).astype(BF16)
    out_ref[...] = feed_forward(
        1, ag2, gain2, gate2, up2, down2, part2, partin2, sq2, sqin2, rs2, rsin2, line2, linein2,
        loads[9:12], None,
    )
    for copy in sends:
        copy.wait_send()


def state_kernel(hid_ref, f_ref, v_ref, state_ref, out_ref, new_ref):
    out_ref[...] = hid_ref[...]
    cols = f_ref[0].T
    for b in range(state_ref.shape[0]):
        value = v_ref[0, b : b + 1, :]
        new_ref[b, 0] = value + cols[:, b : b + 1] * (state_ref[b, 0] - value)


def shards(
    n_kv, n_tp,
    hidden_in, first_gain, first_gate_proj, first_up_proj, first_down_proj, mix_gain,
    query_weight, forget_weight, input_weight, outgate_weight, forget_floor, state_in,
    out_gain, mix_out_weight, second_gain, second_gate_proj, second_up_proj, second_down_proj,
):
    n_l, n_p = split_lines(n_kv)
    rows, width = hidden_in.shape
    units = first_gate_proj.shape[1]
    _, heads, head, _ = state_in.shape
    first_gate_proj, first_up_proj, second_gate_proj, second_up_proj = [
        w.T for w in (first_gate_proj, first_up_proj, second_gate_proj, second_up_proj)
    ]
    v = pltpu.VMEM
    many = n_l * rows
    others = n_tp - 1

    def like(x):
        return v(x.shape, x.dtype)

    def two(shape, dtype):
        return [v(shape, dtype)] * 2

    dma = pltpu.SemaphoreType.DMA
    scratch = (
        [like(x) for x in (
            first_gate_proj, first_up_proj, first_down_proj,
            second_gate_proj, second_up_proj, second_down_proj,
            query_weight, forget_weight, input_weight, outgate_weight, mix_out_weight, state_in)]
        + two((n_kv, rows, width), BF16)
        + two((n_p, 2, many, units), BF16)
        + two((others, n_p, 2, many, units), BF16)
        + [v((n_p, 2, many, units), F32)]
        + two((n_p, many, 128), F32)
        + two((others, n_p, many, 128), F32)
        + two((n_p - 1, n_l, rows, width), BF16)
        + two((n_p - 1, n_l, rows, width), BF16)
        + [v((n_l, rows, width), F32)]
        + two((n_l, rows, width), BF16)
        + two((n_l, rows, width), BF16)
        + [v((n_tp, rows, width), BF16)] * 2
        + [v((others, rows, width), BF16)]
        + [v((heads, rows, head), F32)] * 2
        + [dma((12,)), dma]
        + [dma((2, n_l))] * 2
        + [dma((2, n_l, n_p))] * 2
        + [dma((2, n_p, n_tp))] * 4
        + [dma((2, n_l, n_p))] * 2
        + [dma((2, n_l))] * 2
        + [dma((n_tp,))] * 4
    )
    hbm = pl.BlockSpec(memory_space=pl.ANY)
    vmem = pl.BlockSpec(memory_space=pltpu.VMEM)
    hidden_out, forget, ival = pl.pallas_call(
        functools.partial(step_kernel, n_kv, n_tp),
        out_shape=(
            jax.ShapeDtypeStruct(hidden_in.shape, hidden_in.dtype),
            jax.ShapeDtypeStruct((heads, rows, head), F32),
            jax.ShapeDtypeStruct((heads, rows, head), F32),
        ),
        in_specs=[hbm] + [vmem] * 5 + [hbm] * 12,
        out_specs=(vmem, vmem, vmem),
        scratch_shapes=scratch,
        compiler_params=pltpu.CompilerParams(
            collective_id=0, has_side_effects=True, vmem_limit_bytes=60000 * 1024
        ),
    )(
        hidden_in, first_gain, second_gain, mix_gain, forget_floor, out_gain, first_gate_proj, first_up_proj, first_down_proj,
        query_weight, forget_weight, input_weight, outgate_weight,
        state_in, mix_out_weight, second_gate_proj, second_up_proj, second_down_proj,
    )
    whole = pl.BlockSpec((rows, width), lambda h: (0, 0))
    small = pl.BlockSpec((1, rows, head), lambda h: (h, 0, 0))
    large = pl.BlockSpec((rows, 1, head, head), lambda h: (0, h, 0, 0))
    return pl.pallas_call(
        state_kernel,
        grid=(heads,),
        out_shape=(
            jax.ShapeDtypeStruct(hidden_in.shape, hidden_in.dtype),
            jax.ShapeDtypeStruct(state_in.shape, state_in.dtype),
        ),
        in_specs=[whole, small, small, large],
        out_specs=(whole, large),
    )(hidden_out, forget, ival, state_in)


def solution(mesh):
    placed = (
        P("kv", "tp"), P("tp"), P("tp", "kv"), P("tp", "kv"), P("kv", "tp"), P(),
        P(None, "tp"), P(None, "tp"), P(None, "tp"), P(None, "tp"), P("tp"),
        P("kv", "tp", None, None), P("tp"), P("tp", None), P("tp"),
        P("tp", "kv"), P("tp", "kv"), P("kv", "tp"),
    )
    return jax.shard_map(
        functools.partial(shards, mesh.shape["kv"], mesh.shape["tp"]),
        mesh=mesh,
        in_specs=placed,
        out_specs=(P("kv", "tp"), P("kv", "tp", None, None)),
        check_vma=False,
    )
```
